32 devices in a mesh: sp: 8 (over z, x), tp: 4 (over y, core).
Axes of the slice: x: 2, y: 2, z: 4, core: 2. Of those that a mesh axis runs over, the one named last changes fastest.
Arguments:
- tokens: bfloat16 [1024, 2048], P('sp'), may hold values from -6 to 6
- query_narrow: bfloat16 [1024, 2048], P('sp', 'tp'), may hold values from -20 to 20
- key_narrow: bfloat16 [1024, 2048], P('sp', 'tp'), may hold values from -20 to 20
- value_narrow: bfloat16 [1024, 2048], P('sp', 'tp'), may hold values from -6 to 6
- query_broad: bfloat16 [1024, 4096], P('sp', 'tp'), may hold values from -20 to 20
- key_broad: bfloat16 [1024, 4096], P('sp', 'tp'), may hold values from -20 to 20
- value_broad: bfloat16 [1024, 2048], P('sp', 'tp'), may hold values from -6 to 6
- mix_lambda: float32 [2, 16], P(None, 'tp'), may hold values from 0.3 to 0.8
- head_gain: float32 [2, 128], replicated, may hold values from 0.1 to 1.9
- proj_narrow: bfloat16 [2048, 2048], P('tp'), may hold values from -0.09375 to 0.09375
- proj_broad: bfloat16 [2048, 2048], P('tp'), may hold values from -0.09375 to 0.09375
- gain_one: float32 [2048], replicated, may hold values from 0.1 to 1.9
- gain_two: float32 [2048], replicated, may hold values from 0.1 to 1.9
- expert_ids: int32 [1024, 2], P('sp'), may hold values from 0 to 31, all different within a row; in each aligned block of 128 rows (0 to 127, 128 to 255, ...) at most 16 rows name the same one
- expert_gates: float32 [1024, 2], P('sp'), may hold values from 0.1 to 0.9
- gate_weight: bfloat16 [32, 2048, 4096], P('sp', None, 'tp'), may hold values from -0.125 to 0.125
- up_weight: bfloat16 [32, 2048, 4096], P('sp', None, 'tp'), may hold values from -0.125 to 0.125
- down_weight: bfloat16 [32, 4096, 2048], P('sp', 'tp'), may hold values from -0.09375 to 0.09375
Outputs:
- result: bfloat16 [1024, 2048], P('sp')
The draws below stay inside these ranges and needn't reach their ends.
Inputs may be any that keep to these rules, and one draw needn't show every extreme that they name: `expert_ids`: the 2 experts of a token differ. Among the tokens of one index of sp (aligned blocks of 128 tokens) no expert is named by more than 16 tokens, and in some blocks one expert is named by exactly 16.
All inputs are finite; a program needn't handle non-finite values.
Results may differ from the reference program's by a relative error of at most 0.015.
Values may be sent and summed in bfloat16 or wider, within the bound.
No kernel may reach another device: no remote copies, remote signals or barrier semaphores. Data moves between devices by JAX's collectives and lax.ppermute only.
A program may use at most 128 MiB of HBM per device.

```python
import math
import jax
import jax.numpy as jnp
import numpy as np
from jax import lax

D = 2048
HEADS = 16
QK_NARROW = 64
QK_BROAD = 128
V = 128
EXPERTS = 32
FF_EXP = 4096
TOP = 2
CAP = 16
TOK_DEV = 128
TOKENS = 1024
N_SP = 8
N_TP = 4


def draw_queries(key, key_width, salt):
    base = jax.random.normal(jax.random.fold_in(key, salt), (TOKENS, HEADS, 2, key_width), jnp.float32)
    base = jnp.clip(base * 1.35, -8.0, 8.0)
    return base.reshape(TOKENS, HEADS * 2 * key_width).astype(jnp.bfloat16)


def draw_keys(key, key_width, salt):
    base = jax.random.normal(jax.random.fold_in(key, salt), (TOKENS, HEADS, 2, key_width), jnp.float32)
    base = jnp.clip(base * 1.35, -8.0, 8.0)
    return base.reshape(TOKENS, HEADS * 2 * key_width).astype(jnp.bfloat16)


def draw_query_narrow(key, part):
    return draw_queries(key, QK_NARROW, 31)


def draw_key_narrow(key, part):
    return draw_keys(key, QK_NARROW, 32)


def draw_query_broad(key, part):
    return draw_queries(key, QK_BROAD, 33)


def draw_key_broad(key, part):
    return draw_keys(key, QK_BROAD, 34)


def block_scale(own_key, shape, cuts, least, top_value):
    factor_of, own = 1.0, jax.random.fold_in(own_key, 6)
    for axis_at, blocks in cuts:
        steps = jnp.exp(jax.random.uniform(jax.random.fold_in(own, axis_at), (blocks,), jnp.float32, least / len(cuts), top_value / len(cuts)))
        factor_of = factor_of * jnp.repeat(steps, shape[axis_at] // blocks).reshape([-1 if axis == axis_at else 1 for axis in range(len(shape))])
    return factor_of


def shared_out(own_key, own, number, rows, count, top, most, lean):
    sequence = jax.random.permutation(own_key, count)
    heavy_load, common = portions_of(count, rows * top, most, lean, True), portions_of(count, rows * top, most, lean, False)
    places = jnp.arange(count)

    def named(lengths, rotation):
        used = int((lengths > 0).sum())
        fixed = max(1, used // 4)
        moved = fixed + (places - fixed + rotation * (used - fixed)) % max(1, count - fixed)
        return jnp.zeros((count,), jnp.int32).at[sequence[jnp.where(places < fixed, places, moved)]].set(jnp.asarray(lengths, jnp.int32))

    lengths = jnp.where(number % 4 == 0, named(heavy_load, number // 4), named(common, number - number // 4 - 1))
    mixed = jax.random.permutation(jax.random.fold_in(own, 3), count)
    donor, taker = mixed[0:count // 2 * 2:2], mixed[1:count // 2 * 2:2]
    margin = jnp.minimum(lengths[donor] - 1, most - lengths[taker]) // 2
    margin = jnp.where((donor == sequence[0]) | (taker == sequence[0]) | (lengths[taker] == 0), 0, jnp.maximum(margin, 0))
    moved = jax.random.randint(jax.random.fold_in(own, 4), (count // 2,), 0, 1 << 20) % (margin + 1)
    lengths = lengths.at[donor].add(-moved).at[taker].add(moved)
    items = jnp.searchsorted(jnp.cumsum(lengths), jnp.arange(rows * top), side="right").astype(jnp.int32)
    listing = items.reshape(top, rows).T
    listing = listing[jax.random.permutation(jax.random.fold_in(own, 1), rows)]
    rotation = jax.random.randint(jax.random.fold_in(own, 2), (rows, 1), 0, top)
    return jnp.take_along_axis(listing, (jnp.arange(top)[None, :] + rotation) % top, axis=1)


def portions_of(amount, total, most, lean, full):
    weights = [(1 << 20) // math.isqrt(standing ** lean) + 1 for standing in range(1, amount + 1)]
    largest = most if full else min(most, max(-(-total // amount), total * weights[0] // sum(weights)))
    least = 1 if total - largest >= amount - 1 else 0
    given, spare = [largest] + [least] * (amount - 1), total - largest - least * (amount - 1)
    while spare > 0:
        movable = [i for i in range(1, amount) if given[i] < largest] or [i for i in range(1, amount) if given[i] < most]
        whole, budget = sum([weights[i] for i in movable]), spare
        for i in movable:
            extra = min(most - given[i], max(1, budget * weights[i] // whole), spare)
            given[i] = given[i] + extra
            spare = spare - extra
    return np.array(given)


def noise(own_key, dims, deviation, reach, split=(), kind=jnp.bfloat16):
    level = block_scale(own_key, dims, split, -0.22, 0.18) if split else 1.0
    values = jax.random.normal(own_key, dims, jnp.float32) * deviation * level
    return jnp.minimum(jnp.maximum(values, -reach), reach).astype(kind)


def setup_inputs(seed: int = 0) -> dict:
    arg_keys = jax.random.split(jax.random.key(seed), 19)
    tokens = noise(arg_keys[0], (TOKENS, D), 1.0, 6.0, ((0, 8),))
    query_narrow = draw_query_narrow(jax.random.fold_in(arg_keys[18], 71), 0)
    key_narrow = draw_key_narrow(jax.random.fold_in(arg_keys[18], 71), 0)
    value_narrow = noise(arg_keys[3], (TOKENS, HEADS * V), 1.0, 6.0, ((0, 8), (1, 4)))
    query_broad = draw_query_broad(jax.random.fold_in(arg_keys[18], 71), 0)
    key_broad = draw_key_broad(jax.random.fold_in(arg_keys[18], 71), 0)
    value_broad = noise(arg_keys[6], (TOKENS, HEADS * V), 1.0, 6.0, ((0, 8), (1, 4)))
    mix_lambda = jnp.clip(0.3 + 0.5 * jax.random.uniform(arg_keys[7], (2, HEADS), jnp.float32) ** block_scale(arg_keys[7], (2, HEADS), ((1, 4),), -0.2, 0.2), 0.3, 0.8)
    head_gain = jnp.clip(1.0 + 0.18 * jax.random.normal(arg_keys[8], (2, V), jnp.float32), 0.1, 1.9)
    proj_narrow = noise(arg_keys[9], (HEADS * V, D), (2 * HEADS * V) ** -0.5, 0.09375, ((0, 4),))
    proj_broad = noise(arg_keys[10], (HEADS * V, D), (2 * HEADS * V) ** -0.5, 0.09375, ((0, 4),))
    gain_one = jnp.clip(1.0 + 0.18 * jax.random.normal(arg_keys[11], (D,), jnp.float32), 0.1, 1.9)
    gain_two = jnp.clip(1.0 + 0.18 * jax.random.normal(arg_keys[12], (D,), jnp.float32), 0.1, 1.9)
    expert_ids_keys = jax.random.split(jax.random.fold_in(arg_keys[13], 1), TOKENS // TOK_DEV)
    expert_ids_turns = jax.random.permutation(jax.random.fold_in(arg_keys[13], 3), TOKENS // TOK_DEV)
    expert_ids = jax.vmap(lambda own, number: shared_out(jax.random.fold_in(arg_keys[13], 2), own, number, TOK_DEV, EXPERTS, TOP, CAP, 2))(expert_ids_keys, expert_ids_turns).reshape((TOKENS, TOP))
    expert_gates = jnp.clip(0.1 + 0.79999997 * jax.random.uniform(arg_keys[14], (TOKENS, TOP), jnp.float32) ** block_scale(arg_keys[14], (TOKENS, TOP), ((0, 8),), -0.2, 0.2), 0.1, 0.9)
    gate_weight = noise(arg_keys[15], (EXPERTS, D, FF_EXP), D ** -0.5, 0.125, ((0, 8), (2, 4)))
    up_weight = noise(arg_keys[16], (EXPERTS, D, FF_EXP), D ** -0.5, 0.125, ((0, 8), (2, 4)))
    down_weight = noise(arg_keys[17], (EXPERTS, FF_EXP, D), FF_EXP ** -0.5, 0.09375, ((0, 8), (1, 4)))
    return dict(tokens=tokens, query_narrow=query_narrow, key_narrow=key_narrow, value_narrow=value_narrow, query_broad=query_broad, key_broad=key_broad, value_broad=value_broad, mix_lambda=mix_lambda, head_gain=head_gain, proj_narrow=proj_narrow, proj_broad=proj_broad, gain_one=gain_one, gain_two=gain_two, expert_ids=expert_ids, expert_gates=expert_gates, gate_weight=gate_weight, up_weight=up_weight, down_weight=down_weight)


deep_alpha = 8.0 ** 0.25
norm_eps = 1e-05

def layer_scale(inputs, gains):
    center = lax.optimization_barrier(jnp.mean(inputs, -1, keepdims=True))
    spread = lax.optimization_barrier(jnp.mean(jnp.square(inputs - center), -1, keepdims=True))
    return (inputs - center) * lax.rsqrt(spread + norm_eps) * gains

def group_heads(queries, key_rows, values, mixing, gains, key_width):
    count = queries.shape[0]
    stacked_q = jnp.moveaxis(queries.reshape(count, HEADS, 2, key_width), 1, 0)
    stacked_k = jnp.moveaxis(key_rows.reshape(count, HEADS, 2, key_width), 1, 0)
    stacked_v = jnp.moveaxis(values.reshape(count, HEADS, V), 1, 0)
    factor = key_width ** (-0.5)

    def one_head(members):
        head_q, head_k, head_v, weight = members
        scores = jnp.einsum('qmd,kmd->mqk', head_q.astype(jnp.float32), head_k.astype(jnp.float32)) * factor
        highest = lax.optimization_barrier(jnp.max(scores, -1, keepdims=True))
        exponent = jnp.exp(scores - highest)
        totals = lax.optimization_barrier(jnp.sum(exponent, -1))
        probs = lax.optimization_barrier(exponent.astype(jnp.bfloat16))
        numer = jnp.einsum('mqk,kv->mqv', probs.astype(jnp.float32), head_v.astype(jnp.float32))
        diff = numer[0] / totals[0][:, None] - weight * numer[1] / totals[1][:, None]
        normed = diff * lax.rsqrt(lax.optimization_barrier(jnp.mean(diff * diff, -1, keepdims=True)) + norm_eps) * gains
        return normed.astype(jnp.bfloat16)
    output = lax.map(one_head, (stacked_q, stacked_k, stacked_v, mixing))
    return jnp.moveaxis(output, 0, 1).reshape(count, HEADS * V)

def attention_sum(heads_first, heads_second, proj_narrow, proj_broad):
    count = heads_first.shape[0]
    block_width = HEADS // N_TP * V
    first_blocks = jnp.moveaxis(heads_first.reshape(count, N_TP, block_width), 1, 0)
    second_blocks = jnp.moveaxis(heads_second.reshape(count, N_TP, block_width), 1, 0)
    first_weights = proj_narrow.reshape(N_TP, block_width, D)
    second_weights = proj_broad.reshape(N_TP, block_width, D)

    def add_block(running, members):
        part_one, part_two, weight_one, weight_two = members
        partial_value = jnp.dot(part_one, weight_one, preferred_element_type=jnp.float32)
        partial_value = partial_value + jnp.dot(part_two, weight_two, preferred_element_type=jnp.float32)
        rounded = lax.optimization_barrier(partial_value.astype(jnp.bfloat16))
        return (running + rounded.astype(jnp.float32), None)
    running, _ = lax.scan(add_block, jnp.zeros((count, D), jnp.float32), (first_blocks, second_blocks, first_weights, second_weights))
    return running

def one_expert(members):
    expert_rows, gate_part, up_part, down_part = members
    activated = (jax.nn.silu(jnp.dot(expert_rows, gate_part, preferred_element_type=jnp.float32)) * jnp.dot(expert_rows, up_part, preferred_element_type=jnp.float32)).astype(jnp.bfloat16)
    block_width = FF_EXP // N_TP
    act_blocks = jnp.moveaxis(activated.reshape(expert_rows.shape[0], N_TP, block_width), 1, 0)
    down_blocks = down_part.reshape(N_TP, block_width, D)

    def add_block(running, operands):
        product = jnp.dot(operands[0], operands[1], preferred_element_type=jnp.float32)
        rounded = lax.optimization_barrier(product.astype(jnp.bfloat16))
        return (running + rounded.astype(jnp.float32), None)
    running, _ = lax.scan(add_block, jnp.zeros((expert_rows.shape[0], D), jnp.float32), (act_blocks, down_blocks))
    return running.astype(jnp.bfloat16)

def reference(tokens, query_narrow, key_narrow, value_narrow, query_broad, key_broad, value_broad, mix_lambda, head_gain, proj_narrow, proj_broad, gain_one, gain_two, expert_ids, expert_gates, gate_weight, up_weight, down_weight):
    heads_first = group_heads(query_narrow, key_narrow, value_narrow, mix_lambda[0], head_gain[0], QK_NARROW)
    heads_second = group_heads(query_broad, key_broad, value_broad, mix_lambda[1], head_gain[1], QK_BROAD)
    attn = attention_sum(heads_first, heads_second, proj_narrow, proj_broad)
    mixed_rows = layer_scale(deep_alpha * tokens.astype(jnp.float32) + attn, gain_one).astype(jnp.bfloat16)
    chosen = expert_ids.reshape(N_SP, TOK_DEV * TOP).astype(jnp.int32)
    onehot = (chosen[:, :, None] == jnp.arange(EXPERTS, dtype=jnp.int32)[None, None, :]).astype(jnp.int32)
    before = jnp.cumsum(onehot, axis=1, dtype=jnp.int32) - onehot
    slot_index = lax.optimization_barrier(jnp.sum(before * onehot, axis=-1, dtype=jnp.int32))
    block_index = jnp.arange(N_SP, dtype=jnp.int32)[:, None]
    position = ((chosen * N_SP + block_index) * CAP + slot_index).reshape(-1).astype(jnp.int32)
    repeated = jnp.repeat(mixed_rows, TOP, axis=0)
    buffer = jnp.zeros((EXPERTS * N_SP * CAP, D), jnp.bfloat16).at[position].set(repeated)
    buffer = buffer.reshape(EXPERTS, N_SP * CAP, D)
    outputs = lax.map(one_expert, (buffer, gate_weight, up_weight, down_weight))
    picked = outputs.reshape(EXPERTS * N_SP * CAP, D)[position].reshape(N_SP * TOK_DEV, TOP, D)
    routed = lax.optimization_barrier(jnp.sum(expert_gates[:, :, None] * picked.astype(jnp.float32), axis=1))
    return layer_scale(deep_alpha * mixed_rows.astype(jnp.float32) + routed, gain_two).astype(jnp.bfloat16)
```

```python
import jax
import jax.numpy as jnp
from jax import lax
from jax.experimental import pallas as pl
from jax.experimental.pallas import tpu as pltpu
from jax.sharding import PartitionSpec as P

QK_NARROW = 64
QK_BROAD = 128
V = 128
TOP = 2
CAP = 16


deep_alpha = 8.0**0.25
norm_eps = 1e-05


def layer_scale(inputs, gains):
    center = jnp.mean(inputs, -1, keepdims=True)
    spread = jnp.mean(jnp.square(inputs - center), -1, keepdims=True)
    return (inputs - center) * lax.rsqrt(spread + norm_eps) * gains


def head_fold(running, queries, key_rows, values, key_width):
    maxima, totals, weighted = running
    length = key_rows.shape[0]
    head_count = queries.shape[1]
    keyed = key_rows.reshape(length, head_count, 2, key_width)
    valued = values.reshape(length, head_count, V)
    scores = jnp.einsum(
        "qhmd,khmd->hmqk", queries, keyed, preferred_element_type=jnp.float32
    ) * key_width ** (-0.5)
    updated = jnp.maximum(maxima, jnp.max(scores, -1))
    exponent = jnp.exp(scores - updated[..., None])
    totals = jnp.sum(exponent, -1)
    weighted = jnp.einsum(
        "hmqk,khv->hmqv", exponent.astype(jnp.bfloat16), valued, preferred_element_type=jnp.float32
    )
    return (updated, totals, weighted)


def head_output(running, mixing, gains):
    maxima, totals, weighted = running
    diff = (
        weighted[:, 0] / totals[:, 0, :, None]
        - mixing[:, None, None] * weighted[:, 1] / totals[:, 1, :, None]
    )
    normed = (diff * lax.rsqrt(jnp.mean(diff * diff, -1, keepdims=True) + norm_eps) * gains).astype(
        jnp.bfloat16
    )
    return jnp.moveaxis(normed, 0, 1).reshape(normed.shape[1], -1)


def on_device(
    tokens,
    query_narrow,
    key_narrow,
    value_narrow,
    query_broad,
    key_broad,
    value_broad,
    mix_lambda,
    head_gain,
    proj_narrow,
    proj_broad,
    gain_one,
    gain_two,
    expert_ids,
    expert_gates,
    gate_weight,
    up_weight,
    down_weight,
):
    token_count = tokens.shape[0]
    model_width = tokens.shape[1]
    head_count = value_narrow.shape[1] // V
    queries_first = query_narrow.reshape(token_count, head_count, 2, QK_NARROW)
    queries_second = query_broad.reshape(token_count, head_count, 2, QK_BROAD)
    start_state = (
        jnp.full((head_count, 2, token_count), -1e30, jnp.float32),
        jnp.zeros((head_count, 2, token_count), jnp.float32),
        jnp.zeros((head_count, 2, token_count, V), jnp.float32),
    )
    state_first = head_fold(
        start_state,
        queries_first,
        lax.all_gather(key_narrow, "sp", axis=0, tiled=True),
        lax.all_gather(value_narrow, "sp", axis=0, tiled=True),
        QK_NARROW,
    )
    state_second = head_fold(
        start_state,
        queries_second,
        lax.all_gather(key_broad, "sp", axis=0, tiled=True),
        lax.all_gather(value_broad, "sp", axis=0, tiled=True),
        QK_BROAD,
    )
    heads_first = head_output(state_first, mix_lambda[0], head_gain[0])
    heads_second = head_output(state_second, mix_lambda[1], head_gain[1])
    tp_count = lax.axis_size("tp")
    partial_value = jnp.dot(heads_first, proj_narrow, preferred_element_type=jnp.float32)
    partial_value = partial_value + jnp.dot(
        heads_second, proj_broad, preferred_element_type=jnp.float32
    )
    attn = lax.psum(
        partial_value.astype(jnp.bfloat16).astype(jnp.float32).astype(jnp.bfloat16), "tp"
    ).astype(jnp.float32)
    mixed_rows = layer_scale(deep_alpha * tokens.astype(jnp.float32) + attn, gain_one).astype(
        jnp.bfloat16
    )
    sp_count = lax.axis_size("sp")
    local_experts = gate_weight.shape[0]
    experts_all = local_experts * sp_count
    chosen = expert_ids.reshape(-1)
    onehot = (chosen[:, None] == jnp.arange(experts_all, dtype=jnp.int32)[None, :]).astype(
        jnp.int32
    )
    before = jnp.cumsum(onehot, axis=0, dtype=jnp.int32) - onehot
    slot_index = jnp.sum(before * onehot, axis=-1, dtype=jnp.int32)
    position = slot_index * experts_all + chosen
    repeated = jnp.repeat(mixed_rows, TOP, axis=0)
    outgoing = jnp.zeros((CAP * experts_all, model_width), jnp.bfloat16).at[position].set(repeated)
    outgoing = outgoing.reshape(CAP, experts_all, model_width)
    slot_share = CAP // tp_count
    own_slots = lax.dynamic_slice_in_dim(outgoing, lax.axis_index("tp") * slot_share, slot_share, 0)
    arrived = lax.all_to_all(own_slots, "sp", split_axis=1, concat_axis=1, tiled=True)
    arrived = lax.all_gather(arrived, "tp", axis=0, tiled=True)
    expert_rows = arrived.reshape(CAP * sp_count, local_experts, model_width)
    gated = jnp.einsum("rxd,xdf->rxf", expert_rows, gate_weight, preferred_element_type=jnp.float32)
    lifted = jnp.einsum("rxd,xdf->rxf", expert_rows, up_weight, preferred_element_type=jnp.float32)
    activated = (jax.nn.silu(gated) * lifted).astype(jnp.bfloat16)
    product = jnp.einsum("rxf,xfd->rxd", activated, down_weight, preferred_element_type=jnp.float32)
    summed = lax.psum_scatter(
        product.astype(jnp.bfloat16).astype(jnp.float32).astype(jnp.bfloat16),
        "tp",
        scatter_dimension=0,
        tiled=True,
    )
    returning = summed.reshape(slot_share, sp_count, local_experts, model_width)
    returned = lax.all_to_all(returning, "sp", split_axis=1, concat_axis=1, tiled=True)
    collected = lax.all_gather(returned, "tp", axis=0, tiled=True)
    picked = collected.reshape(CAP * experts_all, model_width)[position].reshape(
        token_count, TOP, model_width
    )
    routed = jnp.sum(expert_gates[:, :, None] * picked.astype(jnp.float32), axis=1)
    return layer_scale(deep_alpha * mixed_rows.astype(jnp.float32) + routed, gain_two).astype(
        jnp.bfloat16
    )


F32, BF16, I32 = jnp.float32, jnp.bfloat16, jnp.int32
MIB = 1 << 20


def exchange(value, axis, step):
    return lax.ppermute(value, axis, [(i, i ^ step) for i in range(lax.axis_size(axis))])


def call(kernel, outs, ins, *, name, flops=1 << 20, vmem=16 * MIB, smem=(), scratch=(), grid=None, in_specs=None, out_specs=None):
    single = not isinstance(outs, list)
    shapes = [outs] if single else outs
    moved = sum(x.size * x.dtype.itemsize for x in list(ins) + shapes)
    specs = in_specs or [
        pl.BlockSpec(memory_space=pltpu.SMEM if i in smem else pltpu.VMEM) for i in range(len(ins))
    ]
    ospecs = out_specs or [pl.BlockSpec(memory_space=pltpu.VMEM) for _ in shapes]
    out = pl.pallas_call(
        kernel,
        out_shape=shapes,
        in_specs=specs,
        out_specs=ospecs,
        scratch_shapes=list(scratch),
        grid=grid or (),
        name=name,
        compiler_params=pltpu.CompilerParams(vmem_limit_bytes=vmem),
        cost_estimate=pl.CostEstimate(flops=flops, bytes_accessed=moved, transcendentals=0),
    )(*ins)
    return out[0] if single else out


def shape(rows, columns, dtype=BF16):
    return jax.ShapeDtypeStruct((rows, columns), dtype)


def head_of(place):
    head = lax.shift_right_logical(place, 1)
    return (head ^ place) & 1, head


def at(start, size, step):
    return pl.ds(pl.multiple_of(start, step), size)


def route_kernel(ids_ref, code_ref, *, experts, cap):
    tokens = ids_ref.shape[1]
    each = lax.broadcasted_iota(I32, (experts, tokens), 0)
    hot = [(each == ids_ref[c : c + 1, :]).astype(F32) for c in range(TOP)]
    earlier = lax.broadcasted_iota(I32, (tokens, tokens), 0) < lax.broadcasted_iota(
        I32, (tokens, tokens), 1
    )
    total = sum(hot[1:], hot[0])
    before = jnp.dot(total.astype(BF16), earlier.astype(BF16), preferred_element_type=F32)
    for c in range(TOP):
        slot = jnp.sum(before * hot[c], axis=0, keepdims=True).astype(I32)
        code_ref[c : c + 1, :] = ids_ref[c : c + 1, :] * cap + slot


def pack_kernel(qn, kn, vn, qb, kb, vb, *outs):
    me = lax.axis_index("sp")
    low = lax.broadcasted_iota(I32, (qn.shape[0], V), 1) < QK_NARROW
    for k, out in enumerate(outs):
        group, head = head_of(me ^ k)
        one = at(head * V, V, V)

        @pl.when(group == 0)
        def _():
            queries, keys = qn[:, one], kn[:, one]
            none = jnp.zeros_like(queries)
            out[:, 0:V] = jnp.where(low, queries, none)
            out[:, V : 2 * V] = keys
            out[:, 2 * V : 3 * V] = jnp.where(low, none, queries)
            out[:, 3 * V : 4 * V] = keys
            out[:, 4 * V : 5 * V] = vn[:, one]

        @pl.when(group == 1)
        def _():
            first, second = at(head * 2 * V, V, V), at(head * 2 * V + V, V, V)
            out[:, 0:V] = qb[:, first]
            out[:, V : 2 * V] = kb[:, first]
            out[:, 2 * V : 3 * V] = qb[:, second]
            out[:, 3 * V : 4 * V] = kb[:, second]
            out[:, 4 * V : 5 * V] = vb[:, one]


def attend_kernel(count, *refs):
    blocks, (mix_ref, gain_ref), outs = refs[:count], refs[count : count + 2], refs[count + 2 :]
    group, head = head_of(lax.axis_index("sp"))
    wide = group == 1
    scale = jnp.where(wide, QK_BROAD**-0.5, QK_NARROW**-0.5).astype(F32)
    weight = mix_ref[group, head]
    gains = jnp.where(wide, gain_ref[1:2, :], gain_ref[0:1, :])

    def joined(column, which):
        return jnp.concatenate([blocks[k][:, column * V : column * V + V] for k in which], 0)

    everyone = range(count)
    keys = joined(1, everyone), joined(3, everyone)
    values = joined(4, everyone)

    def one_map(queries, keyed):
        scores = lax.dot_general(queries, keyed, (((1,), (1,)), ((), ())), preferred_element_type=F32)
        top = jnp.max(scores, -1, keepdims=True)
        expo = jnp.exp((scores - top) * scale)
        total = jnp.sum(expo, -1, keepdims=True)
        numer = jnp.dot(expo.astype(BF16), values, preferred_element_type=F32)
        return numer / total

    for i, out in enumerate(outs):
        pair = (2 * i, 2 * i + 1)
        diff = one_map(joined(0, pair), keys[0]) - weight * one_map(joined(2, pair), keys[1])
        spread = jnp.mean(diff * diff, -1, keepdims=True)
        out[...] = (diff * lax.rsqrt(spread + norm_eps) * gains).astype(BF16)


def project_kernel(count, *refs):
    pairs = refs[: count // 2]
    mates_ref, narrow_ref, broad_ref, send_ref, keep_ref, heads = refs[count // 2 :]
    me, core = lax.axis_index("sp"), lax.axis_index("tp") & 1
    half = send_ref.shape[0]
    width = narrow_ref.shape[0]

    @pl.when(pl.program_id(0) == 0)
    def _():
        for k in range(count):
            group, head = head_of(me ^ k)
            column = at(group * width + head * V, V, V)
            for part, owner in ((0, 1 - core), (1, core)):
                rows = at(owner * half, half, half)
                block = (
                    pairs[k // 2][rows, :]
                    if k % 2 == 0
                    else mates_ref[rows, (k // 2) * V : (k // 2) * V + V]
                )
                heads[part * half : part * half + half, column] = block

    total = jnp.dot(heads[:, :width], narrow_ref[...], preferred_element_type=F32)
    total = total + jnp.dot(heads[:, width:], broad_ref[...], preferred_element_type=F32)
    send_ref[...] = total[:half].astype(BF16)
    keep_ref[...] = total[half:].astype(BF16)


def normed(value, gains):
    center = jnp.mean(value, -1, keepdims=True)
    away = value - center
    spread = jnp.mean(away * away, -1, keepdims=True)
    return away * lax.rsqrt(spread + norm_eps) * gains


def mixed_kernel(one_ref, two_ref, token_ref, gain_ref, out_ref):
    half = out_ref.shape[0]
    core = lax.axis_index("tp") & 1
    rows = token_ref[at(core * half, half, half), :].astype(F32)
    attn = one_ref[...].astype(F32) + two_ref[...].astype(F32)
    out_ref[...] = normed(deep_alpha * rows + attn, gain_ref[...]).astype(BF16)


def row_codes(count, rows, share, cap, experts):
    me, core = lax.axis_index("sp"), lax.axis_index("tp") & 1
    row = lax.broadcasted_iota(I32, (count * rows, 1), 0)
    step = row // rows
    inner = row - step * rows
    local = inner // share
    return ((me ^ step) * experts + local) * cap + core * share + inner - local * share


def dispatch_kernel(cap, experts, mine_ref, other_ref, code_ref, *refs):
    outs, whole = refs[:-1], refs[-1]
    count, rows = len(outs), outs[0].shape[0]
    half = mine_ref.shape[0]
    core = lax.axis_index("tp") & 1
    whole[at(core * half, half, half), :] = mine_ref[...]
    whole[at((1 - core) * half, half, half), :] = other_ref[...]
    codes = row_codes(count, rows, rows // experts, cap, experts)
    chosen = sum([(codes == code_ref[c : c + 1, :]).astype(F32) for c in range(TOP)])
    sent = jnp.dot(chosen.astype(BF16), whole[...], preferred_element_type=F32).astype(BF16)
    for k, out in enumerate(outs):
        out[...] = sent[k * rows : k * rows + rows]


def gather_kernel(experts, *refs):
    blocks, out = refs[:-1], refs[-1]
    share = blocks[0].shape[0] // experts
    for e in range(experts):
        for k, block in enumerate(blocks):
            start = (e * len(blocks) + k) * share
            out[start : start + share, :] = block[e * share : e * share + share, :]


def expert_kernel(mine_ref, mate_ref, gate_ref, up_ref, down_ref, keep_ref, send_ref, total):
    step = pl.program_id(1)
    rows = mine_ref.shape[0]
    given = jnp.concatenate([mine_ref[...], mate_ref[...]], 0)
    gated = jnp.dot(given, gate_ref[0], preferred_element_type=F32)
    lifted = jnp.dot(given, up_ref[0], preferred_element_type=F32)
    act = (gated / (1.0 + jnp.exp(-gated)) * lifted).astype(BF16)
    down = jnp.dot(act, down_ref[0], preferred_element_type=F32)

    @pl.when(step == 0)
    def _():
        total[...] = down

    @pl.when(step != 0)
    def _():
        total[...] += down

    @pl.when(step == pl.num_programs(1) - 1)
    def _():
        keep_ref[...] = total[:rows].astype(BF16)
        send_ref[...] = total[rows:].astype(BF16)


def spread_kernel(experts, keep_ref, got_ref, *outs):
    share = outs[0].shape[0] // experts
    for e in range(experts):
        for k, out in enumerate(outs):
            rows = slice((e * len(outs) + k) * share, (e * len(outs) + k) * share + share)
            both = keep_ref[rows, :].astype(F32) + got_ref[rows, :].astype(F32)
            out[e * share : e * share + share, :] = both.astype(BF16)


def combine_kernel(cap, experts, *refs):
    count = len(refs) - 5
    blocks, (code_ref, gate_ref, send_ref, keep_ref, total) = refs[:count], refs[count:]
    rows = blocks[0].shape[0]
    half = send_ref.shape[0]
    core = lax.axis_index("tp") & 1
    codes = row_codes(count, rows, rows // experts, cap, experts)
    weights = sum(
        [jnp.where(codes == code_ref[c : c + 1, :], gate_ref[c : c + 1, :], 0.0) for c in range(TOP)]
    )
    high = weights.astype(BF16)
    low = (weights - high.astype(F32)).astype(BF16)
    given = jnp.concatenate([block[...] for block in blocks], 0)
    over_rows = (((0,), (0,)), ((), ()))
    total[...] = lax.dot_general(high, given, over_rows, preferred_element_type=F32)
    total[...] += lax.dot_general(low, given, over_rows, preferred_element_type=F32)
    send_ref[...] = total[at((1 - core) * half, half, half), :].astype(BF16)
    keep_ref[...] = total[at(core * half, half, half), :].astype(BF16)


def final_kernel(one_ref, two_ref, mixed_ref, gain_ref, out_ref):
    routed = one_ref[...].astype(F32) + two_ref[...].astype(F32)
    rows = mixed_ref[...].astype(F32)
    out_ref[...] = normed(deep_alpha * rows + routed, gain_ref[...]).astype(BF16)


def join_kernel(mine_ref, other_ref, out_ref):
    half = mine_ref.shape[0]
    core = lax.axis_index("tp") & 1
    out_ref[at(core * half, half, half), :] = mine_ref[...]
    out_ref[at((1 - core) * half, half, half), :] = other_ref[...]


def add(one, two):
    return (one.astype(F32) + two.astype(F32)).astype(BF16)


def fast(
    tokens, query_narrow, key_narrow, value_narrow, query_broad, key_broad, value_broad, mix_lambda,
    head_gain, proj_narrow, proj_broad, gain_one, gain_two, expert_ids, expert_gates, gate_weight,
    up_weight, down_weight,
):
    import functools

    part = functools.partial
    count = lax.axis_size("sp")
    token_count, width = tokens.shape
    half = token_count // 2
    experts, _, hidden = gate_weight.shape
    share = CAP // 2
    rows = experts * share

    ids, gates = expert_ids.T, expert_gates.T
    codes = call(
        part(route_kernel, experts=experts * count, cap=CAP),
        jax.ShapeDtypeStruct(ids.shape, I32), [ids], name="route",
    )
    sent = call(
        pack_kernel, [shape(token_count, 5 * V)] * count,
        [query_narrow, key_narrow, value_narrow, query_broad, key_broad, value_broad], name="pack",
    )
    blocks = [sent[0]] + [exchange(sent[k], "sp", k) for k in range(1, count)]
    outs = call(
        part(attend_kernel, count), [shape(2 * token_count, V)] * (count // 2),
        blocks + [mix_lambda, head_gain], smem=(count,), name="attend", vmem=32 * MIB, flops=1 << 31,
    )
    pairs = [outs[0]] + [exchange(outs[i], "sp", 2 * i) for i in range(1, count // 2)]
    mates = exchange(jnp.concatenate([p[token_count:] for p in pairs], 1), "sp", 1)
    tile = width // 4
    whole = lambda x: pl.BlockSpec(x.shape, lambda i: (0, 0))
    send, keep = call(
        part(project_kernel, count), [shape(half, width)] * 2, pairs + [mates, proj_narrow, proj_broad],
        name="project", flops=1 << 29, grid=(width // tile,),
        in_specs=[whole(x) for x in pairs + [mates]]
        + [pl.BlockSpec((proj_narrow.shape[0], tile), lambda i: (0, i))] * 2,
        out_specs=[pl.BlockSpec((half, tile), lambda i: (0, i))] * 2,
        scratch=[pltpu.VMEM((token_count, 2 * proj_narrow.shape[0]), BF16)],
    )
    chip = add(keep, exchange(send, "tp", 1))
    mixed = call(
        mixed_kernel, shape(half, width),
        [chip, exchange(chip, "tp", 2), tokens, gain_one.reshape(1, -1)], name="mixed",
    )
    others = exchange(mixed, "tp", 1)
    sent = call(
        part(dispatch_kernel, CAP, experts), [shape(rows, width)] * count, [mixed, others, codes],
        name="dispatch", scratch=[pltpu.VMEM((token_count, width), BF16)],
    )
    blocks = [sent[0]] + [exchange(sent[k], "sp", k) for k in range(1, count)]
    mine = call(part(gather_kernel, experts), shape(rows * count, width), blocks, name="gather")
    mate = exchange(mine, "tp", 1)
    each = share * count
    step = hidden // 4
    keep, send = call(
        expert_kernel, [shape(rows * count, width)] * 2, [mine, mate, gate_weight, up_weight, down_weight],
        name="experts", flops=1 << 33, vmem=32 * MIB, grid=(experts, hidden // step),
        in_specs=[pl.BlockSpec((each, width), lambda e, f: (e, 0))] * 2
        + [pl.BlockSpec((1, width, step), lambda e, f: (e, 0, f))] * 2
        + [pl.BlockSpec((1, step, width), lambda e, f: (e, f, 0))],
        out_specs=[pl.BlockSpec((each, width), lambda e, f: (e, 0))] * 2,
        scratch=[pltpu.VMEM((2 * each, width), F32)],
    )
    got = exchange(send, "tp", 1)
    sent = call(part(spread_kernel, experts), [shape(rows, width)] * count, [keep, got], name="spread")
    blocks = [sent[0]] + [exchange(sent[k], "sp", k) for k in range(1, count)]
    send, keep = call(
        part(combine_kernel, CAP, experts), [shape(half, width)] * 2, blocks + [codes, gates],
        name="combine", scratch=[pltpu.VMEM((token_count, width), F32)],
    )
    chip = add(keep, exchange(send, "tp", 1))
    result = call(
        final_kernel, shape(half, width), [chip, exchange(chip, "tp", 2), mixed, gain_two.reshape(1, -1)],
        name="final",
    )
    return call(join_kernel, shape(token_count, width), [result, exchange(result, "tp", 1)], name="join")


def layer(*args):
    tokens, value_narrow, ids = args[0], args[3], args[13]
    count, tp_count = lax.axis_size("sp"), lax.axis_size("tp")
    fits = (
        tp_count == 4
        and count == 2 * (value_narrow.shape[1] // V)
        and count & (count - 1) == 0
        and QK_BROAD == V
        and 2 * QK_NARROW == V
        and tokens.shape[0] % 16 == 0
        and ids.shape[1] == TOP
    )
    return (fast if fits else on_device)(*args)


def solution(mesh):
    return jax.shard_map(
        layer,
        mesh=mesh,
        in_specs=(
            P("sp", None),
            P("sp", "tp"),
            P("sp", "tp"),
            P("sp", "tp"),
            P("sp", "tp"),
            P("sp", "tp"),
            P("sp", "tp"),
            P(None, "tp"),
            P(),
            P("tp", None),
            P("tp", None),
            P(),
            P(),
            P("sp", None),
            P("sp", None),
            P("sp", None, "tp"),
            P("sp", None, "tp"),
            P("sp", "tp", None),
        ),
        out_specs=P("sp", None),
        check_vma=False,
    )
```

```python
import functools
import math

import jax
import jax.numpy as jnp
from jax import lax
from jax.experimental import pallas as pl
from jax.experimental.pallas import tpu as pltpu
from jax.sharding import PartitionSpec as P

QK_NARROW = 64
QK_BROAD = 128
V = 128
TOP = 2
CAP = 16


deep_alpha = 8.0**0.25
norm_eps = 1e-05


def layer_scale(inputs, gains):
    center = jnp.mean(inputs, -1, keepdims=True)
    spread = jnp.mean(jnp.square(inputs - center), -1, keepdims=True)
    return (inputs - center) * lax.rsqrt(spread + norm_eps) * gains


def head_fold(running, queries, key_rows, values, key_width):
    maxima, totals, weighted = running
    length = key_rows.shape[0]
    head_count = queries.shape[1]
    keyed = key_rows.reshape(length, head_count, 2, key_width)
    valued = values.reshape(length, head_count, V)
    scores = jnp.einsum(
        "qhmd,khmd->hmqk", queries, keyed, preferred_element_type=jnp.float32
    ) * key_width ** (-0.5)
    updated = jnp.maximum(maxima, jnp.max(scores, -1))
    exponent = jnp.exp(scores - updated[..., None])
    totals = jnp.sum(exponent, -1)
    weighted = jnp.einsum(
        "hmqk,khv->hmqv", exponent.astype(jnp.bfloat16), valued, preferred_element_type=jnp.float32
    )
    return (updated, totals, weighted)


def head_output(running, mixing, gains):
    _, totals, weighted = running
    diff = (
        weighted[:, 0] / totals[:, 0, :, None]
        - mixing[:, None, None] * weighted[:, 1] / totals[:, 1, :, None]
    )
    normed = (diff * lax.rsqrt(jnp.mean(diff * diff, -1, keepdims=True) + norm_eps) * gains).astype(
        jnp.bfloat16
    )
    return jnp.moveaxis(normed, 0, 1).reshape(normed.shape[1], -1)


def on_device(
    tokens,
    query_narrow,
    key_narrow,
    value_narrow,
    query_broad,
    key_broad,
    value_broad,
    mix_lambda,
    head_gain,
    proj_narrow,
    proj_broad,
    gain_one,
    gain_two,
    expert_ids,
    expert_gates,
    gate_weight,
    up_weight,
    down_weight,
):
    token_count = tokens.shape[0]
    model_width = tokens.shape[1]
    head_count = value_narrow.shape[1] // V
    queries_first = query_narrow.reshape(token_count, head_count, 2, QK_NARROW)
    queries_second = query_broad.reshape(token_count, head_count, 2, QK_BROAD)
    start_state = (
        jnp.full((head_count, 2, token_count), -1e30, jnp.float32),
        jnp.zeros((head_count, 2, token_count), jnp.float32),
        jnp.zeros((head_count, 2, token_count, V), jnp.float32),
    )
    state_first = head_fold(
        start_state,
        queries_first,
        lax.all_gather(key_narrow, "sp", axis=0, tiled=True),
        lax.all_gather(value_narrow, "sp", axis=0, tiled=True),
        QK_NARROW,
    )
    state_second = head_fold(
        start_state,
        queries_second,
        lax.all_gather(key_broad, "sp", axis=0, tiled=True),
        lax.all_gather(value_broad, "sp", axis=0, tiled=True),
        QK_BROAD,
    )
    heads_first = head_output(state_first, mix_lambda[0], head_gain[0])
    heads_second = head_output(state_second, mix_lambda[1], head_gain[1])
    tp_count = lax.axis_size("tp")
    partial_value = jnp.dot(heads_first, proj_narrow, preferred_element_type=jnp.float32)
    partial_value = partial_value + jnp.dot(
        heads_second, proj_broad, preferred_element_type=jnp.float32
    )
    attn = lax.psum(
        partial_value.astype(jnp.bfloat16).astype(jnp.float32).astype(jnp.bfloat16), "tp"
    ).astype(jnp.float32)
    mixed_rows = layer_scale(deep_alpha * tokens.astype(jnp.float32) + attn, gain_one).astype(
        jnp.bfloat16
    )
    sp_count = lax.axis_size("sp")
    local_experts = gate_weight.shape[0]
    experts_all = local_experts * sp_count
    chosen = expert_ids.reshape(-1)
    onehot = (chosen[:, None] == jnp.arange(experts_all, dtype=jnp.int32)[None, :]).astype(
        jnp.int32
    )
    before = jnp.cumsum(onehot, axis=0, dtype=jnp.int32) - onehot
    slot_index = jnp.sum(before * onehot, axis=-1, dtype=jnp.int32)
    position = slot_index * experts_all + chosen
    repeated = jnp.repeat(mixed_rows, TOP, axis=0)
    outgoing = jnp.zeros((CAP * experts_all, model_width), jnp.bfloat16).at[position].set(repeated)
    outgoing = outgoing.reshape(CAP, experts_all, model_width)
    slot_share = CAP // tp_count
    own_slots = lax.dynamic_slice_in_dim(outgoing, lax.axis_index("tp") * slot_share, slot_share, 0)
    arrived = lax.all_to_all(own_slots, "sp", split_axis=1, concat_axis=1, tiled=True)
    arrived = lax.all_gather(arrived, "tp", axis=0, tiled=True)
    expert_rows = arrived.reshape(CAP * sp_count, local_experts, model_width)
    gated = jnp.einsum("rxd,xdf->rxf", expert_rows, gate_weight, preferred_element_type=jnp.float32)
    lifted = jnp.einsum("rxd,xdf->rxf", expert_rows, up_weight, preferred_element_type=jnp.float32)
    activated = (jax.nn.silu(gated) * lifted).astype(jnp.bfloat16)
    product = jnp.einsum("rxf,xfd->rxd", activated, down_weight, preferred_element_type=jnp.float32)
    summed = lax.psum_scatter(
        product.astype(jnp.bfloat16).astype(jnp.float32).astype(jnp.bfloat16),
        "tp",
        scatter_dimension=0,
        tiled=True,
    )
    returning = summed.reshape(slot_share, sp_count, local_experts, model_width)
    returned = lax.all_to_all(returning, "sp", split_axis=1, concat_axis=1, tiled=True)
    collected = lax.all_gather(returned, "tp", axis=0, tiled=True)
    picked = collected.reshape(CAP * experts_all, model_width)[position].reshape(
        token_count, TOP, model_width
    )
    routed = jnp.sum(expert_gates[:, :, None] * picked.astype(jnp.float32), axis=1)
    return layer_scale(deep_alpha * mixed_rows.astype(jnp.float32) + routed, gain_two).astype(
        jnp.bfloat16
    )


F32, BF16, I32 = jnp.float32, jnp.bfloat16, jnp.int32
MIB = 1 << 20


def exchange(value, axis, step):
    return lax.ppermute(value, axis, [(i, i ^ step) for i in range(lax.axis_size(axis))])


def call(kernel, outs, ins, *, flops=1 << 20, vmem=8 * MIB, hbm=(), held=(), scratch=(), grid=None, in_specs=None, out_specs=None):
    single = not isinstance(outs, list)
    shapes = [outs] if single else outs
    ins = [pltpu.with_memory_space_constraint(x, pltpu.HBM) if i in hbm else x for i, x in enumerate(ins)]
    ins = [pltpu.with_memory_space_constraint(x, pltpu.VMEM) if i in held else x for i, x in enumerate(ins)]
    moved = sum(math.prod(x.shape) * x.dtype.itemsize for x in list(ins) + shapes)
    specs = in_specs or [
        pl.BlockSpec(memory_space=pltpu.HBM if i in hbm else pltpu.VMEM) for i in range(len(ins))
    ]
    ospecs = out_specs or [pl.BlockSpec(memory_space=pltpu.VMEM) for _ in shapes]
    out = pl.pallas_call(
        kernel,
        out_shape=shapes,
        in_specs=specs,
        out_specs=ospecs,
        scratch_shapes=list(scratch),
        grid=grid or (),
        compiler_params=pltpu.CompilerParams(vmem_limit_bytes=vmem),
        cost_estimate=pl.CostEstimate(flops=flops, bytes_accessed=moved, transcendentals=0),
    )(*ins)
    return out[0] if single else list(out)


def shape(rows, columns, dtype=BF16):
    return jax.ShapeDtypeStruct((rows, columns), dtype)


def head_of(place):
    head = lax.shift_right_logical(place, 1)
    return (head ^ place) & 1, head


def at(start, size, step):
    return pl.ds(pl.multiple_of(start, step), size)


def fetch(pairs, sems):
    copies = [pltpu.make_async_copy(a, b, sems.at[i]) for i, (a, b) in enumerate(pairs)]
    for copy in copies:
        copy.start()
    return copies


def pack_kernel(*refs):
    sources, outs, (sems, *held) = refs[:6], refs[6:-7], refs[-7:]
    for copy in fetch(list(zip(sources, held)), sems):
        copy.wait()
    qn, kn, vn, qb, kb, vb = held
    me = lax.axis_index("sp")
    low = lax.broadcasted_iota(I32, (qn.shape[0], V), 1) < QK_NARROW
    for k, out in enumerate(outs):
        group, head = head_of(me ^ k)
        one = at(head * V, V, V)

        @pl.when(group == 0)
        def _():
            queries, keys = qn[:, one], kn[:, one]
            none = jnp.zeros_like(queries)
            out[:, 0:V] = jnp.where(low, queries, none)
            out[:, V : 2 * V] = keys
            out[:, 2 * V : 3 * V] = jnp.where(low, none, queries)
            out[:, 3 * V : 4 * V] = keys
            out[:, 4 * V : 5 * V] = vn[:, one]

        @pl.when(group == 1)
        def _():
            first, second = at(head * 2 * V, V, V), at(head * 2 * V + V, V, V)
            out[:, 0:V] = qb[:, first]
            out[:, V : 2 * V] = kb[:, first]
            out[:, 2 * V : 3 * V] = qb[:, second]
            out[:, 3 * V : 4 * V] = kb[:, second]
            out[:, 4 * V : 5 * V] = vb[:, one]


def prepare_kernel(experts, cap, *refs):
    ids_hbm, mix_hbm, gain_hbm, *sources = refs[:10]
    code_ref, coef_ref, *kept = refs[11:-5]
    sems, ids_ref, mix_ref, gain_ref, more = refs[-5:]
    core = lax.axis_index("tp") & 1
    half = kept[2].shape[0]
    views = [
        sources[0],
        sources[1],
        sources[2].at[at(core * half, half, half)],
        sources[3],
    ] + [sources[4 + i % 3].at[pl.ds(i // 3, 1)] for i in range(len(kept) - 4)]
    others = fetch(list(zip(views, kept)), more)
    for copy in fetch([(ids_hbm, ids_ref), (mix_hbm, mix_ref), (gain_hbm, gain_ref)], sems):
        copy.wait()
    tokens = ids_ref.shape[1]
    each = lax.broadcasted_iota(I32, (experts, tokens), 0)
    hot = [(each == ids_ref[c : c + 1, :]).astype(F32) for c in range(TOP)]
    earlier = lax.broadcasted_iota(I32, (tokens, tokens), 0) < lax.broadcasted_iota(
        I32, (tokens, tokens), 1
    )
    before = jnp.dot(
        sum(hot[1:], hot[0]).astype(BF16), earlier.astype(F32).astype(BF16), preferred_element_type=F32
    )
    for c in range(TOP):
        slot = jnp.sum(before * hot[c], axis=0, keepdims=True).astype(I32)
        code_ref[c : c + 1, :] = ids_ref[c : c + 1, :] * cap + slot
    group, head = head_of(lax.axis_index("sp"))
    here = (lax.broadcasted_iota(I32, mix_ref.shape, 0) == group) & (
        lax.broadcasted_iota(I32, mix_ref.shape, 1) == head
    )
    weight = jnp.sum(jnp.sum(jnp.where(here, mix_ref[...], 0.0), -1, keepdims=True), 0, keepdims=True)
    coef_ref[0:1, :] = jnp.where(group == 1, gain_ref[1:2, :], gain_ref[0:1, :])
    coef_ref[1:2, :] = jnp.broadcast_to(weight, (1, coef_ref.shape[1]))
    for copy in others:
        copy.wait()


def attend_kernel(count, chosen, *refs):
    blocks, coef_ref, outs = refs[:count], refs[count], refs[count + 1 :]
    group, _ = head_of(lax.axis_index("sp"))
    scale = jnp.where(group == 1, QK_BROAD**-0.5, QK_NARROW**-0.5).astype(F32)
    gains, weight = coef_ref[0:1, :], coef_ref[1:2, :]

    def joined(column, which):
        return jnp.concatenate([blocks[k][:, column * V : column * V + V] for k in which], 0)

    everyone = range(count)
    keys = joined(1, everyone), joined(3, everyone)
    values = joined(4, everyone)

    def one_map(queries, keyed):
        scores = lax.dot_general(queries, keyed, (((1,), (1,)), ((), ())), preferred_element_type=F32)
        top = jnp.max(scores, -1, keepdims=True)
        expo = jnp.exp((scores - top) * scale)
        total = jnp.sum(expo, -1, keepdims=True)
        numer = jnp.dot(expo.astype(BF16), values, preferred_element_type=F32)
        return numer / total

    rows = blocks[0].shape[0]
    for i in range(0, len(chosen), 2):
        pair = chosen[i : i + 2]
        diff = one_map(joined(0, pair), keys[0]) - weight * one_map(joined(2, pair), keys[1])
        spread = jnp.mean(diff * diff, -1, keepdims=True)
        result = (diff * lax.rsqrt(spread + norm_eps) * gains).astype(BF16)
        for n in range(len(pair)):
            outs[0][:, (i + n) * V : (i + n) * V + V] = result[n * rows : n * rows + rows]


def project_kernel(count, *refs):
    pairs, (narrow_ref, broad_ref, send_ref, keep_ref, heads) = refs[: count // 2], refs[count // 2 :]
    me, core = lax.axis_index("sp"), lax.axis_index("tp") & 1
    half, width = send_ref.shape[0], narrow_ref.shape[0]
    for k in range(count):
        group, head = head_of(me ^ k)
        column = at(group * width + head * V, V, V)
        side = (k % 2) * V
        for part, owner in ((0, 1 - core), (1, core)):
            block = pairs[k // 2][at(owner * half, half, half), side : side + V]
            heads[part * half : part * half + half, column] = block
    tile = send_ref.shape[1] // 4
    for i in range(4):
        columns = slice(i * tile, i * tile + tile)
        total = jnp.dot(heads[:, :width], narrow_ref[:, columns], preferred_element_type=F32)
        total = total + jnp.dot(heads[:, width:], broad_ref[:, columns], preferred_element_type=F32)
        send_ref[:, columns] = total[:half].astype(BF16)
        keep_ref[:, columns] = total[half:].astype(BF16)


def normed(value, gains):
    center = jnp.mean(value, -1, keepdims=True)
    away = value - center
    spread = jnp.mean(away * away, -1, keepdims=True)
    return away * lax.rsqrt(spread + norm_eps) * gains


def mixed_kernel(one_ref, two_ref, row_ref, gain_ref, out_ref):
    attn = one_ref[...].astype(F32) + two_ref[...].astype(F32)
    out_ref[...] = normed(deep_alpha * row_ref[...].astype(F32) + attn, gain_ref[...]).astype(BF16)


def row_codes(cap, experts, share, steps, chosen, first):
    me, core = lax.axis_index("sp"), lax.axis_index("tp") & 1
    rows = chosen * share
    row = lax.broadcasted_iota(I32, (len(steps) * rows, 1), 0)
    step = row // rows
    inner = row - step * rows
    local = inner // share
    return ((me ^ (step + steps[0])) * experts + first + local) * cap + core * share + inner - local * share


def all_codes(cap, experts, share, count):
    part = experts // 2
    chip = lax.shift_right_logical(lax.axis_index("tp"), 1)
    near, far = range(count // 2), range(count // 2, count)
    return jnp.concatenate(
        [row_codes(cap, experts, share, near, experts, 0), row_codes(cap, experts, share, far, part, chip * part)], 0
    )


def dispatch_kernel(cap, experts, mine_ref, other_ref, code_ref, *refs):
    outs, whole = refs[:-1], refs[-1]
    count = len(outs)
    half = mine_ref.shape[0]
    core = lax.axis_index("tp") & 1
    whole[at(core * half, half, half), :] = mine_ref[...]
    whole[at((1 - core) * half, half, half), :] = other_ref[...]
    codes = all_codes(cap, experts, outs[0].shape[0] // experts, count)
    chosen = sum([(codes == code_ref[c : c + 1, :]).astype(F32) for c in range(TOP)])
    sent = jnp.dot(chosen.astype(BF16), whole[...], preferred_element_type=F32).astype(BF16)
    start = 0
    for out in outs:
        out[...] = sent[start : start + out.shape[0]]
        start += out.shape[0]


def stack_kernel(experts, *refs):
    blocks, (near_ref, far_ref) = refs[:-2], refs[-2:]
    near = len(blocks) // 2
    share = blocks[0].shape[0] // experts
    for e in range(experts):
        for k in range(near):
            start = (e * near + k) * share
            near_ref[start : start + share, :] = blocks[k][e * share : e * share + share, :]
    rows = blocks[near].shape[0]
    for k in range(near):
        far_ref[k * rows : k * rows + rows, :] = blocks[near + k][...]


def expert_kernel(near, *refs):
    rows_in, first, later = refs[:6], refs[6:-11], refs[-11:-8]
    keep_near, keep_far, send_near, send_far, sems, *slots = refs[-8:]
    ready, streamed = len(first) // 3, slots[0].shape[0]
    copies = [
        fetch([(x.at[ready + e], y.at[e]) for x, y in zip(later, slots)], sems.at[e]) for e in range(streamed)
    ]
    experts = ready + streamed
    part = experts // 2
    each = rows_in[0].shape[0] // experts
    share = each // near
    tile = first[0].shape[2] // 4
    chip = lax.shift_right_logical(lax.axis_index("tp"), 1)
    for e in range(experts):
        held, n = (first[3 * e : 3 * e + 3], 0) if e < ready else (slots, e - ready)
        if e >= ready:
            for copy in copies[n]:
                copy.wait()
        own, local = chip == e // part, e % part
        rows = slice(e * each, e * each + each)
        places = [(k * part + local) * share for k in range(near)]
        given = []
        for near_ref, mine_ref, other_ref in (rows_in[:3], rows_in[3:]):
            given.append(near_ref[rows, :])
            for p in places:
                given.append(jnp.where(own, mine_ref[p : p + share, :], other_ref[p : p + share, :]))
        given = jnp.concatenate(given, 0)
        acts = []
        for f in range(4):
            columns = slice(f * tile, f * tile + tile)
            gated = jnp.dot(given, held[0][n, :, columns], preferred_element_type=F32)
            lifted = jnp.dot(given, held[1][n, :, columns], preferred_element_type=F32)
            acts.append((gated / (1.0 + jnp.exp(-gated)) * lifted).astype(BF16))
        total = jnp.dot(jnp.concatenate(acts, 1), held[2][n], preferred_element_type=F32).astype(BF16)
        half = keep_far.shape[0] // 2
        base = jnp.where(own, half, 0)
        for near_ref, far_ref, start in ((keep_near, keep_far, 0), (send_near, send_far, 2 * each)):
            near_ref[rows, :] = total[start : start + each]
            for k, p in enumerate(places):
                source = start + each + k * share
                far_ref[at(base + p, share, share), :] = total[source : source + share]


def sum_far_kernel(keep_ref, got_ref, *outs):
    start = 0
    for out in outs:
        rows = slice(start, start + out.shape[0])
        out[...] = (keep_ref[rows, :].astype(F32) + got_ref[rows, :].astype(F32)).astype(BF16)
        start += out.shape[0]


def sum_near_kernel(experts, keep_ref, got_ref, *outs):
    share = outs[0].shape[0] // experts
    for e in range(experts):
        for k, out in enumerate(outs):
            start = (e * len(outs) + k) * share
            rows = slice(start, start + share)
            out[e * share : e * share + share, :] = (
                keep_ref[rows, :].astype(F32) + got_ref[rows, :].astype(F32)
            ).astype(BF16)


def split_kernel(offset, mine_ref, got_ref, *outs):
    rows = outs[0].shape[0]
    for k, out in enumerate(outs):
        own = mine_ref[offset + k * rows : offset + k * rows + rows, :].astype(F32)
        out[...] = (own + got_ref[k * rows : k * rows + rows, :].astype(F32)).astype(BF16)


def combine_kernel(cap, experts, *refs):
    count = len(refs) - 5
    blocks, (code_ref, gate_ref, send_ref, keep_ref, total) = refs[:count], refs[count:]
    half = send_ref.shape[0]
    core = lax.axis_index("tp") & 1
    codes = all_codes(cap, experts, blocks[0].shape[0] // experts, count)
    weights = sum(
        [jnp.where(codes == code_ref[c : c + 1, :], gate_ref[c : c + 1, :], 0.0) for c in range(TOP)]
    )
    high = weights.astype(BF16)
    low = (weights - high.astype(F32)).astype(BF16)
    given = jnp.concatenate([block[...] for block in blocks], 0)
    over_rows = (((0,), (0,)), ((), ()))
    total[...] = lax.dot_general(high, given, over_rows, preferred_element_type=F32)
    total[...] += lax.dot_general(low, given, over_rows, preferred_element_type=F32)
    send_ref[...] = total[at((1 - core) * half, half, half), :].astype(BF16)
    keep_ref[...] = total[at(core * half, half, half), :].astype(BF16)


def final_kernel(one_ref, two_ref, mixed_ref, gain_ref, out_ref):
    routed = one_ref[...].astype(F32) + two_ref[...].astype(F32)
    rows = mixed_ref[...].astype(F32)
    out_ref[...] = normed(deep_alpha * rows + routed, gain_ref[...]).astype(BF16)


def join_kernel(mine_ref, other_ref, out_ref):
    half = mine_ref.shape[0]
    core = lax.axis_index("tp") & 1
    out_ref[at(core * half, half, half), :] = mine_ref[...]
    out_ref[at((1 - core) * half, half, half), :] = other_ref[...]


def add(one, two):
    return (one.astype(F32) + two.astype(F32)).astype(BF16)


def fast(
    tokens, query_narrow, key_narrow, value_narrow, query_broad, key_broad, value_broad, mix_lambda,
    head_gain, proj_narrow, proj_broad, gain_one, gain_two, expert_ids, expert_gates, gate_weight,
    up_weight, down_weight,
):
    part = functools.partial
    count = lax.axis_size("sp")
    token_count, width = tokens.shape
    half = token_count // 2
    experts, _, _ = gate_weight.shape
    share = CAP // 2
    rows = experts * share

    ids, gates = expert_ids.T, expert_gates.T
    everyone, near, far = range(count), range(count // 2), range(count // 2, count)
    DMA = pltpu.SemaphoreType.DMA
    given = [query_narrow, key_narrow, value_narrow, query_broad, key_broad, value_broad]
    sent = call(
        pack_kernel, [shape(token_count, 5 * V)] * count, given, hbm=range(6),
        scratch=[DMA((6,))] + [pltpu.VMEM(x.shape, BF16) for x in given],
    )
    ready = experts * 3 // 4
    weights = [gate_weight, up_weight, down_weight]
    here = [proj_narrow, proj_broad, shape(half, width), shape(1, width, F32)] + [
        jax.ShapeDtypeStruct((1,) + x.shape[1:], BF16) for x in weights * ready
    ]
    codes, coef, narrow, broad, row, gain, *first = call(
        part(prepare_kernel, experts * count, CAP),
        [jax.ShapeDtypeStruct(ids.shape, I32), shape(2, V, F32)] + [pltpu.VMEM(x.shape, x.dtype) for x in here],
        [ids, mix_lambda, head_gain, proj_narrow, proj_broad, tokens, gain_one.reshape(1, -1)] + weights + [sent[0]],
        hbm=range(10), flops=1 << 33, vmem=4 * MIB,
        scratch=[DMA((3,)), pltpu.VMEM(ids.shape, I32), pltpu.VMEM(mix_lambda.shape, F32), pltpu.VMEM(head_gain.shape, F32), DMA((4 + 3 * ready,))],
    )
    blocks = [sent[0]] + [exchange(sent[k], "sp", k) for k in everyone[1:]]

    def attend(chosen):
        return call(
            part(attend_kernel, count, chosen), shape(token_count, len(chosen) * V), blocks + [coef],
            vmem=9 * MIB, flops=len(chosen) << 28,
        )

    theirs = exchange(attend(everyone[1::2]), "sp", 1)
    ours = attend(everyone[0::2])
    pairs = [
        jnp.concatenate([ours[:, i * V : i * V + V], theirs[:, i * V : i * V + V]], 1) for i in near
    ]
    pairs = [pairs[0]] + [exchange(pairs[i], "sp", 2 * i) for i in near[1:]]
    inner = proj_narrow.shape[0]
    send, keep = call(
        part(project_kernel, count), [shape(half, width)] * 2, pairs + [narrow, broad],
        flops=1 << 29, held=range(count // 2, count // 2 + 2), scratch=[pltpu.VMEM((token_count, 2 * inner), BF16)],
    )
    chip = add(keep, exchange(send, "tp", 1))
    mixed = call(mixed_kernel, shape(half, width), [chip, exchange(chip, "tp", 2), row, gain], held=(2, 3))
    others = exchange(mixed, "tp", 1)
    sizes = [shape(rows, width)] * len(near) + [shape(rows // 2, width)] * len(far)
    sent = call(
        part(dispatch_kernel, CAP, experts), sizes, [mixed, others, codes],
        scratch=[pltpu.VMEM((token_count, width), BF16)],
    )
    distant = [exchange(sent[k], "sp", k) for k in far]
    blocks = [sent[0]] + [exchange(sent[k], "sp", k) for k in near[1:]] + distant
    sizes = [shape(rows * len(near), width), shape(rows // 2 * len(far), width)]
    mine = call(part(stack_kernel, experts), sizes, blocks)
    other = exchange(mine[1], "tp", 2)
    mate = [exchange(x, "tp", 1) for x in mine]
    streamed = experts - ready
    kept = [shape(x.shape[0] * f, width) for x, f in zip(sizes, (1, 2))]
    keep_near, keep_far, send_near, send_far = call(
        part(expert_kernel, len(near)), [pltpu.VMEM(x.shape, BF16) for x in kept * 2],
        mine + [other] + mate + [exchange(other, "tp", 1)] + first + weights,
        flops=1 << 33, vmem=14 * MIB, held=range(6 + len(first)), hbm=range(6 + len(first), 9 + len(first)),
        scratch=[DMA((streamed, 3))] + [pltpu.VMEM((streamed,) + x.shape[1:], BF16) for x in weights],
    )
    got_far, got_near = exchange(send_far, "tp", 1), exchange(send_near, "tp", 1)
    pieces = 2
    piece = sizes[1].shape[0] // pieces
    *others, distant = call(sum_far_kernel, [shape(piece, width)] * pieces + [sizes[1]], [keep_far, got_far])
    others = [exchange(x, "tp", 2) for x in others]
    sent = call(part(sum_near_kernel, experts), [shape(rows, width)] * len(near), [keep_near, got_near])
    blocks = [sent[0]] + [exchange(sent[k], "sp", k) for k in near[1:]]
    span = len(far) // pieces
    for n in range(pieces):
        sent = call(part(split_kernel, n * piece), [shape(rows // 2, width)] * span, [distant, others[n]])
        blocks += [exchange(x, "sp", k) for x, k in zip(sent, far[n * span : n * span + span])]
    send, keep = call(
        part(combine_kernel, CAP, experts), [shape(half, width)] * 2, blocks + [codes, gates],
        scratch=[pltpu.VMEM((token_count, width), F32)],
    )
    chip = add(keep, exchange(send, "tp", 1))
    result = call(final_kernel, shape(half, width), [chip, exchange(chip, "tp", 2), mixed, gain_two.reshape(1, -1)])
    return call(join_kernel, shape(token_count, width), [result, exchange(result, "tp", 1)])


def layer(*args):
    tokens, value_narrow, ids = args[0], args[3], args[13]
    count, tp_count = lax.axis_size("sp"), lax.axis_size("tp")
    fits = (
        tp_count == 4
        and count == 2 * (value_narrow.shape[1] // V)
        and count & (count - 1) == 0
        and QK_BROAD == V
        and 2 * QK_NARROW == V
        and tokens.shape[0] % 16 == 0
        and ids.shape[1] == TOP
        and args[15].shape[0] % 2 == 0
    )
    return (fast if fits else on_device)(*args)


def solution(mesh):
    return jax.shard_map(
        layer,
        mesh=mesh,
        in_specs=(
            P("sp", None),
            P("sp", "tp"),
            P("sp", "tp"),
            P("sp", "tp"),
            P("sp", "tp"),
            P("sp", "tp"),
            P("sp", "tp"),
            P(None, "tp"),
            P(),
            P("tp", None),
            P("tp", None),
            P(),
            P(),
            P("sp", None),
            P("sp", None),
            P("sp", None, "tp"),
            P("sp", None, "tp"),
            P("sp", "tp", None),
        ),
        out_specs=P("sp", None),
        check_vma=False,
    )
```

```python
import functools
import math

import jax
import jax.numpy as jnp
from jax import lax
from jax.experimental import pallas as pl
from jax.experimental.pallas import tpu as pltpu
from jax.sharding import PartitionSpec as P

QK_NARROW = 64
QK_BROAD = 128
V = 128
TOP = 2
CAP = 16


deep_alpha = 8.0**0.25
norm_eps = 1e-05


def layer_scale(inputs, gains):
    center = jnp.mean(inputs, -1, keepdims=True)
    spread = jnp.mean(jnp.square(inputs - center), -1, keepdims=True)
    return (inputs - center) * lax.rsqrt(spread + norm_eps) * gains


def head_fold(running, queries, key_rows, values, key_width):
    maxima, totals, weighted = running
    length = key_rows.shape[0]
    head_count = queries.shape[1]
    keyed = key_rows.reshape(length, head_count, 2, key_width)
    valued = values.reshape(length, head_count, V)
    scores = jnp.einsum(
        "qhmd,khmd->hmqk", queries, keyed, preferred_element_type=jnp.float32
    ) * key_width ** (-0.5)
    updated = jnp.maximum(maxima, jnp.max(scores, -1))
    exponent = jnp.exp(scores - updated[..., None])
    totals = jnp.sum(exponent, -1)
    weighted = jnp.einsum(
        "hmqk,khv->hmqv", exponent.astype(jnp.bfloat16), valued, preferred_element_type=jnp.float32
    )
    return (updated, totals, weighted)


def head_output(running, mixing, gains):
    _, totals, weighted = running
    diff = (
        weighted[:, 0] / totals[:, 0, :, None]
        - mixing[:, None, None] * weighted[:, 1] / totals[:, 1, :, None]
    )
    normed = (diff * lax.rsqrt(jnp.mean(diff * diff, -1, keepdims=True) + norm_eps) * gains).astype(
        jnp.bfloat16
    )
    return jnp.moveaxis(normed, 0, 1).reshape(normed.shape[1], -1)


def on_device(
    tokens,
    query_narrow,
    key_narrow,
    value_narrow,
    query_broad,
    key_broad,
    value_broad,
    mix_lambda,
    head_gain,
    proj_narrow,
    proj_broad,
    gain_one,
    gain_two,
    expert_ids,
    expert_gates,
    gate_weight,
    up_weight,
    down_weight,
):
    token_count = tokens.shape[0]
    model_width = tokens.shape[1]
    head_count = value_narrow.shape[1] // V
    queries_first = query_narrow.reshape(token_count, head_count, 2, QK_NARROW)
    queries_second = query_broad.reshape(token_count, head_count, 2, QK_BROAD)
    start_state = (
        jnp.full((head_count, 2, token_count), -1e30, jnp.float32),
        jnp.zeros((head_count, 2, token_count), jnp.float32),
        jnp.zeros((head_count, 2, token_count, V), jnp.float32),
    )
    state_first = head_fold(
        start_state,
        queries_first,
        lax.all_gather(key_narrow, "sp", axis=0, tiled=True),
        lax.all_gather(value_narrow, "sp", axis=0, tiled=True),
        QK_NARROW,
    )
    state_second = head_fold(
        start_state,
        queries_second,
        lax.all_gather(key_broad, "sp", axis=0, tiled=True),
        lax.all_gather(value_broad, "sp", axis=0, tiled=True),
        QK_BROAD,
    )
    heads_first = head_output(state_first, mix_lambda[0], head_gain[0])
    heads_second = head_output(state_second, mix_lambda[1], head_gain[1])
    tp_count = lax.axis_size("tp")
    partial_value = jnp.dot(heads_first, proj_narrow, preferred_element_type=jnp.float32)
    partial_value = partial_value + jnp.dot(
        heads_second, proj_broad, preferred_element_type=jnp.float32
    )
    attn = lax.psum(
        partial_value.astype(jnp.bfloat16).astype(jnp.float32).astype(jnp.bfloat16), "tp"
    ).astype(jnp.float32)
    mixed_rows = layer_scale(deep_alpha * tokens.astype(jnp.float32) + attn, gain_one).astype(
        jnp.bfloat16
    )
    sp_count = lax.axis_size("sp")
    local_experts = gate_weight.shape[0]
    experts_all = local_experts * sp_count
    chosen = expert_ids.reshape(-1)
    onehot = (chosen[:, None] == jnp.arange(experts_all, dtype=jnp.int32)[None, :]).astype(
        jnp.int32
    )
    before = jnp.cumsum(onehot, axis=0, dtype=jnp.int32) - onehot
    slot_index = jnp.sum(before * onehot, axis=-1, dtype=jnp.int32)
    position = slot_index * experts_all + chosen
    repeated = jnp.repeat(mixed_rows, TOP, axis=0)
    outgoing = jnp.zeros((CAP * experts_all, model_width), jnp.bfloat16).at[position].set(repeated)
    outgoing = outgoing.reshape(CAP, experts_all, model_width)
    slot_share = CAP // tp_count
    own_slots = lax.dynamic_slice_in_dim(outgoing, lax.axis_index("tp") * slot_share, slot_share, 0)
    arrived = lax.all_to_all(own_slots, "sp", split_axis=1, concat_axis=1, tiled=True)
    arrived = lax.all_gather(arrived, "tp", axis=0, tiled=True)
    expert_rows = arrived.reshape(CAP * sp_count, local_experts, model_width)
    gated = jnp.einsum("rxd,xdf->rxf", expert_rows, gate_weight, preferred_element_type=jnp.float32)
    lifted = jnp.einsum("rxd,xdf->rxf", expert_rows, up_weight, preferred_element_type=jnp.float32)
    activated = (jax.nn.silu(gated) * lifted).astype(jnp.bfloat16)
    product = jnp.einsum("rxf,xfd->rxd", activated, down_weight, preferred_element_type=jnp.float32)
    summed = lax.psum_scatter(
        product.astype(jnp.bfloat16).astype(jnp.float32).astype(jnp.bfloat16),
        "tp",
        scatter_dimension=0,
        tiled=True,
    )
    returning = summed.reshape(slot_share, sp_count, local_experts, model_width)
    returned = lax.all_to_all(returning, "sp", split_axis=1, concat_axis=1, tiled=True)
    collected = lax.all_gather(returned, "tp", axis=0, tiled=True)
    picked = collected.reshape(CAP * experts_all, model_width)[position].reshape(
        token_count, TOP, model_width
    )
    routed = jnp.sum(expert_gates[:, :, None] * picked.astype(jnp.float32), axis=1)
    return layer_scale(deep_alpha * mixed_rows.astype(jnp.float32) + routed, gain_two).astype(
        jnp.bfloat16
    )


F32, BF16, I32 = jnp.float32, jnp.bfloat16, jnp.int32
MIB = 1 << 20
WHOLE = 5


def exchange(value, axis, step):
    return lax.ppermute(value, axis, [(i, i ^ step) for i in range(lax.axis_size(axis))])


def call(kernel, outs, ins, *, flops=1 << 20, vmem=8 * MIB, hbm=(), held=(), scratch=(), grid=None, in_specs=None, out_specs=None):
    single = not isinstance(outs, list)
    shapes = [outs] if single else outs
    ins = [pltpu.with_memory_space_constraint(x, pltpu.HBM) if i in hbm else x for i, x in enumerate(ins)]
    ins = [pltpu.with_memory_space_constraint(x, pltpu.VMEM) if i in held else x for i, x in enumerate(ins)]
    moved = sum(math.prod(x.shape) * x.dtype.itemsize for x in list(ins) + shapes)
    specs = in_specs or [
        pl.BlockSpec(memory_space=pltpu.HBM if i in hbm else pltpu.VMEM) for i in range(len(ins))
    ]
    ospecs = out_specs or [pl.BlockSpec(memory_space=pltpu.VMEM) for _ in shapes]
    out = pl.pallas_call(
        kernel,
        out_shape=shapes,
        in_specs=specs,
        out_specs=ospecs,
        scratch_shapes=list(scratch),
        grid=grid or (),
        compiler_params=pltpu.CompilerParams(vmem_limit_bytes=vmem),
        cost_estimate=pl.CostEstimate(flops=flops, bytes_accessed=moved, transcendentals=0),
    )(*ins)
    return out[0] if single else list(out)


def shape(rows, columns, dtype=BF16):
    return jax.ShapeDtypeStruct((rows, columns), dtype)


def head_of(place):
    head = lax.shift_right_logical(place, 1)
    return (head ^ place) & 1, head


def at(start, size, step):
    return pl.ds(pl.multiple_of(start, step), size)


def fetch(pairs, sems):
    copies = [pltpu.make_async_copy(a, b, sems.at[i]) for i, (a, b) in enumerate(pairs)]
    for copy in copies:
        copy.start()
    return copies


def pack_kernel(*refs):
    sources, outs, (sems, *held) = refs[:6], refs[6:-7], refs[-7:]
    for copy in fetch(list(zip(sources, held)), sems):
        copy.wait()
    qn, kn, vn, qb, kb, vb = held
    me = lax.axis_index("sp")
    low = lax.broadcasted_iota(I32, (qn.shape[0], V), 1) < QK_NARROW
    for k, out in enumerate(outs):
        group, head = head_of(me ^ k)
        one = at(head * V, V, V)

        @pl.when(group == 0)
        def _():
            queries, keys = qn[:, one], kn[:, one]
            none = jnp.zeros_like(queries)
            out[:, 0:V] = jnp.where(low, queries, none)
            out[:, V : 2 * V] = keys
            out[:, 2 * V : 3 * V] = jnp.where(low, none, queries)
            out[:, 3 * V : 4 * V] = keys
            out[:, 4 * V : 5 * V] = vn[:, one]

        @pl.when(group == 1)
        def _():
            first, second = at(head * 2 * V, V, V), at(head * 2 * V + V, V, V)
            out[:, 0:V] = qb[:, first]
            out[:, V : 2 * V] = kb[:, first]
            out[:, 2 * V : 3 * V] = qb[:, second]
            out[:, 3 * V : 4 * V] = kb[:, second]
            out[:, 4 * V : 5 * V] = vb[:, one]


def prepare_kernel(experts, cap, *refs):
    ids_hbm, mix_hbm, gain_hbm, *sources = refs[:10]
    code_ref, coef_ref, *kept = refs[11:-5]
    sems, ids_ref, mix_ref, gain_ref, more = refs[-5:]
    core = lax.axis_index("tp") & 1
    half = kept[2].shape[0]
    views = [
        sources[0],
        sources[1],
        sources[2].at[at(core * half, half, half)],
        sources[3],
    ] + [sources[4 + i % 3].at[pl.ds(i // 3, 1)] for i in range(len(kept) - 4)]
    others = fetch(list(zip(views, kept)), more)
    for copy in fetch([(ids_hbm, ids_ref), (mix_hbm, mix_ref), (gain_hbm, gain_ref)], sems):
        copy.wait()
    tokens = ids_ref.shape[1]
    each = lax.broadcasted_iota(I32, (experts, tokens), 0)
    hot = [(each == ids_ref[c : c + 1, :]).astype(F32) for c in range(TOP)]
    earlier = lax.broadcasted_iota(I32, (tokens, tokens), 0) < lax.broadcasted_iota(
        I32, (tokens, tokens), 1
    )
    before = jnp.dot(
        sum(hot[1:], hot[0]).astype(BF16), earlier.astype(F32).astype(BF16), preferred_element_type=F32
    )
    for c in range(TOP):
        slot = jnp.sum(before * hot[c], axis=0, keepdims=True).astype(I32)
        code_ref[c : c + 1, :] = ids_ref[c : c + 1, :] * cap + slot
    group, head = head_of(lax.axis_index("sp"))
    here = (lax.broadcasted_iota(I32, mix_ref.shape, 0) == group) & (
        lax.broadcasted_iota(I32, mix_ref.shape, 1) == head
    )
    weight = jnp.sum(jnp.sum(jnp.where(here, mix_ref[...], 0.0), -1, keepdims=True), 0, keepdims=True)
    coef_ref[0:1, :] = jnp.where(group == 1, gain_ref[1:2, :], gain_ref[0:1, :])
    coef_ref[1:2, :] = jnp.broadcast_to(weight, (1, coef_ref.shape[1]))
    for copy in others:
        copy.wait()


def attend_kernel(count, chosen, *refs):
    blocks, coef_ref, outs = refs[:count], refs[count], refs[count + 1 :]
    group, _ = head_of(lax.axis_index("sp"))
    scale = jnp.where(group == 1, QK_BROAD**-0.5, QK_NARROW**-0.5).astype(F32)
    gains, weight = coef_ref[0:1, :], coef_ref[1:2, :]

    def joined(column, which):
        return jnp.concatenate([blocks[k][:, column * V : column * V + V] for k in which], 0)

    everyone = range(count)
    keys = joined(1, everyone), joined(3, everyone)
    values = joined(4, everyone)

    def one_map(queries, keyed):
        scores = lax.dot_general(queries, keyed, (((1,), (1,)), ((), ())), preferred_element_type=F32)
        top = jnp.max(scores, -1, keepdims=True)
        expo = jnp.exp((scores - top) * scale)
        total = jnp.sum(expo, -1, keepdims=True)
        numer = jnp.dot(expo.astype(BF16), values, preferred_element_type=F32)
        return numer / total

    rows = blocks[0].shape[0]
    for i in range(0, len(chosen), 2):
        pair = chosen[i : i + 2]
        diff = one_map(joined(0, pair), keys[0]) - weight * one_map(joined(2, pair), keys[1])
        spread = jnp.mean(diff * diff, -1, keepdims=True)
        result = (diff * lax.rsqrt(spread + norm_eps) * gains).astype(BF16)
        for n in range(len(pair)):
            outs[0][:, (i + n) * V : (i + n) * V + V] = result[n * rows : n * rows + rows]


def project_kernel(count, *refs):
    pairs, (narrow_ref, broad_ref, send_ref, keep_ref, heads) = refs[: count // 2], refs[count // 2 :]
    me, core = lax.axis_index("sp"), lax.axis_index("tp") & 1
    half, width = send_ref.shape[0], narrow_ref.shape[0]
    for k in range(count):
        group, head = head_of(me ^ k)
        column = at(group * width + head * V, V, V)
        side = (k % 2) * V
        for part, owner in ((0, 1 - core), (1, core)):
            block = pairs[k // 2][at(owner * half, half, half), side : side + V]
            heads[part * half : part * half + half, column] = block
    tile = send_ref.shape[1] // 4
    for i in range(4):
        columns = slice(i * tile, i * tile + tile)
        total = jnp.dot(heads[:, :width], narrow_ref[:, columns], preferred_element_type=F32)
        total = total + jnp.dot(heads[:, width:], broad_ref[:, columns], preferred_element_type=F32)
        send_ref[:, columns] = total[:half].astype(BF16)
        keep_ref[:, columns] = total[half:].astype(BF16)


def normed(value, gains):
    center = jnp.mean(value, -1, keepdims=True)
    away = value - center
    spread = jnp.mean(away * away, -1, keepdims=True)
    return away * lax.rsqrt(spread + norm_eps) * gains


def mixed_kernel(one_ref, two_ref, row_ref, gain_ref, out_ref):
    attn = one_ref[...].astype(F32) + two_ref[...].astype(F32)
    out_ref[...] = normed(deep_alpha * row_ref[...].astype(F32) + attn, gain_ref[...]).astype(BF16)


def row_codes(cap, experts, share, steps, chosen, first):
    me, core = lax.axis_index("sp"), lax.axis_index("tp") & 1
    rows = chosen * share
    row = lax.broadcasted_iota(I32, (len(steps) * rows, 1), 0)
    step = row // rows
    inner = row - step * rows
    local = inner // share
    return ((me ^ (step + steps[0])) * experts + first + local) * cap + core * share + inner - local * share


def all_codes(cap, experts, share, count, split):
    part = experts // 2
    chip = lax.shift_right_logical(lax.axis_index("tp"), 1)
    near, far = range(split), range(split, count)
    return jnp.concatenate(
        [row_codes(cap, experts, share, near, experts, 0), row_codes(cap, experts, share, far, part, chip * part)], 0
    )


def dispatch_kernel(cap, experts, mine_ref, other_ref, code_ref, *refs):
    outs, whole = refs[:-1], refs[-1]
    count = len(outs)
    half = mine_ref.shape[0]
    core = lax.axis_index("tp") & 1
    whole[at(core * half, half, half), :] = mine_ref[...]
    whole[at((1 - core) * half, half, half), :] = other_ref[...]
    codes = all_codes(cap, experts, outs[0].shape[0] // experts, count, count // 2)
    chosen = sum([(codes == code_ref[c : c + 1, :]).astype(F32) for c in range(TOP)])
    sent = jnp.dot(chosen.astype(BF16), whole[...], preferred_element_type=F32).astype(BF16)
    start = 0
    for out in outs:
        out[...] = sent[start : start + out.shape[0]]
        start += out.shape[0]


def stack_kernel(experts, near, *refs):
    blocks, far_ref = refs[: -2 if near else -1], refs[-1]
    for e in range(experts if near else 0):
        share = blocks[0].shape[0] // experts
        for k in range(near):
            start = (e * near + k) * share
            refs[-2][start : start + share, :] = blocks[k][e * share : e * share + share, :]
    rows = blocks[-1].shape[0]
    for k, block in enumerate(blocks[near:]):
        far_ref[k * rows : k * rows + rows, :] = block[...]


def expert_kernel(near, *refs):
    rows_in, first, later = refs[:10], refs[10:-11], refs[-11:-8]
    keep_near, keep_far, send_near, send_far, sems, *slots = refs[-8:]
    ready, streamed = len(first) // 3, slots[0].shape[0]
    copies = [
        fetch([(x.at[ready + e], y.at[e]) for x, y in zip(later, slots)], sems.at[e]) for e in range(streamed)
    ]
    experts = ready + streamed
    part = experts // 2
    each = rows_in[0].shape[0] // experts
    share = each // near
    tile = first[0].shape[2] // 4
    chip = lax.shift_right_logical(lax.axis_index("tp"), 1)
    for e in range(experts):
        held, n = (first[3 * e : 3 * e + 3], 0) if e < ready else (slots, e - ready)
        if e >= ready:
            for copy in copies[n]:
                copy.wait()
        own, local = chip == e // part, e % part
        rows = slice(e * each, e * each + each)
        given = []
        for near_ref, *pieces in (rows_in[:5], rows_in[5:]):
            given.append(near_ref[rows, :])
            for k in range(near):
                first_half, inside = k < near // 2, k % (near // 2)
                mine_ref, other_ref = pieces[:2] if first_half else pieces[2:]
                p = (inside * part + local) * share
                given.append(jnp.where(own, mine_ref[p : p + share, :], other_ref[p : p + share, :]))
        given = jnp.concatenate(given, 0)
        acts = []
        for f in range(4):
            columns = slice(f * tile, f * tile + tile)
            gated = jnp.dot(given, held[0][n, :, columns], preferred_element_type=F32)
            lifted = jnp.dot(given, held[1][n, :, columns], preferred_element_type=F32)
            acts.append((gated / (1.0 + jnp.exp(-gated)) * lifted).astype(BF16))
        total = jnp.dot(jnp.concatenate(acts, 1), held[2][n], preferred_element_type=F32).astype(BF16)
        half = keep_far.shape[0] // 2
        base = jnp.where(own, half, 0)
        size = keep_near.shape[0] // experts
        for near_ref, far_ref, start in ((keep_near, keep_far, 0), (send_near, send_far, 2 * each)):
            near_ref[e * size : e * size + size, :] = total[start : start + size]
            for k in range(half // (part * share)):
                source = start + size + k * share
                far_ref[at(base + (k * part + local) * share, share, share), :] = total[source : source + share]


def sum_far_kernel(keep_ref, got_ref, *outs):
    start = 0
    for out in outs:
        rows = slice(start, start + out.shape[0])
        out[...] = (keep_ref[rows, :].astype(F32) + got_ref[rows, :].astype(F32)).astype(BF16)
        start += out.shape[0]


def sum_near_kernel(experts, keep_ref, got_ref, *outs):
    share = outs[0].shape[0] // experts
    for e in range(experts):
        for k, out in enumerate(outs):
            start = (e * len(outs) + k) * share
            rows = slice(start, start + share)
            out[e * share : e * share + share, :] = (
                keep_ref[rows, :].astype(F32) + got_ref[rows, :].astype(F32)
            ).astype(BF16)


def split_kernel(offset, mine_ref, got_ref, *outs):
    rows = outs[0].shape[0]
    for k, out in enumerate(outs):
        own = mine_ref[offset + k * rows : offset + k * rows + rows, :].astype(F32)
        out[...] = (own + got_ref[k * rows : k * rows + rows, :].astype(F32)).astype(BF16)


def combine_kernel(cap, experts, split, *refs):
    count = len(refs) - 5
    blocks, (code_ref, gate_ref, send_ref, keep_ref, total) = refs[:count], refs[count:]
    half = send_ref.shape[0]
    core = lax.axis_index("tp") & 1
    codes = all_codes(cap, experts, blocks[0].shape[0] // experts, count, split)
    weights = sum(
        [jnp.where(codes == code_ref[c : c + 1, :], gate_ref[c : c + 1, :], 0.0) for c in range(TOP)]
    )
    high = weights.astype(BF16)
    low = (weights - high.astype(F32)).astype(BF16)
    given = jnp.concatenate([block[...] for block in blocks], 0)
    over_rows = (((0,), (0,)), ((), ()))
    total[...] = lax.dot_general(high, given, over_rows, preferred_element_type=F32)
    total[...] += lax.dot_general(low, given, over_rows, preferred_element_type=F32)
    send_ref[...] = total[at((1 - core) * half, half, half), :].astype(BF16)
    keep_ref[...] = total[at(core * half, half, half), :].astype(BF16)


def final_kernel(one_ref, two_ref, mixed_ref, gain_ref, out_ref):
    routed = one_ref[...].astype(F32) + two_ref[...].astype(F32)
    rows = mixed_ref[...].astype(F32)
    out_ref[...] = normed(deep_alpha * rows + routed, gain_ref[...]).astype(BF16)


def join_kernel(mine_ref, other_ref, out_ref):
    half = mine_ref.shape[0]
    core = lax.axis_index("tp") & 1
    out_ref[at(core * half, half, half), :] = mine_ref[...]
    out_ref[at((1 - core) * half, half, half), :] = other_ref[...]


def add(one, two):
    return (one.astype(F32) + two.astype(F32)).astype(BF16)


def fast(
    tokens, query_narrow, key_narrow, value_narrow, query_broad, key_broad, value_broad, mix_lambda,
    head_gain, proj_narrow, proj_broad, gain_one, gain_two, expert_ids, expert_gates, gate_weight,
    up_weight, down_weight,
):
    part = functools.partial
    count = lax.axis_size("sp")
    token_count, width = tokens.shape
    half = token_count // 2
    experts, _, _ = gate_weight.shape
    share = CAP // 2
    rows = experts * share

    ids, gates = expert_ids.T, expert_gates.T
    everyone, near, far = range(count), range(count // 2), range(count // 2, count)
    DMA = pltpu.SemaphoreType.DMA
    given = [query_narrow, key_narrow, value_narrow, query_broad, key_broad, value_broad]
    sent = call(
        pack_kernel, [shape(token_count, 5 * V)] * count, given, hbm=range(6),
        scratch=[DMA((6,))] + [pltpu.VMEM(x.shape, BF16) for x in given],
    )
    ready = experts * 3 // 4
    weights = [gate_weight, up_weight, down_weight]
    here = [proj_narrow, proj_broad, shape(half, width), shape(1, width, F32)] + [
        jax.ShapeDtypeStruct((1,) + x.shape[1:], BF16) for x in weights * ready
    ]
    codes, coef, narrow, broad, row, gain, *first = call(
        part(prepare_kernel, experts * count, CAP),
        [jax.ShapeDtypeStruct(ids.shape, I32), shape(2, V, F32)] + [pltpu.VMEM(x.shape, x.dtype) for x in here],
        [ids, mix_lambda, head_gain, proj_narrow, proj_broad, tokens, gain_one.reshape(1, -1)] + weights + [sent[0]],
        hbm=range(10), flops=1 << 33, vmem=4 * MIB,
        scratch=[DMA((3,)), pltpu.VMEM(ids.shape, I32), pltpu.VMEM(mix_lambda.shape, F32), pltpu.VMEM(head_gain.shape, F32), DMA((4 + 3 * ready,))],
    )
    blocks = [sent[0]] + [exchange(sent[k], "sp", k) for k in everyone[1:]]

    def attend(chosen):
        return call(
            part(attend_kernel, count, chosen), shape(token_count, len(chosen) * V), blocks + [coef],
            vmem=9 * MIB, flops=len(chosen) << 28,
        )

    theirs = exchange(attend(everyone[1::2]), "sp", 1)
    ours = attend(everyone[0::2])
    pairs = [
        jnp.concatenate([ours[:, i * V : i * V + V], theirs[:, i * V : i * V + V]], 1) for i in near
    ]
    pairs = [pairs[0]] + [exchange(pairs[i], "sp", 2 * i) for i in near[1:]]
    inner = proj_narrow.shape[0]
    send, keep = call(
        part(project_kernel, count), [shape(half, width)] * 2, pairs + [narrow, broad],
        flops=1 << 29, held=range(count // 2, count // 2 + 2), scratch=[pltpu.VMEM((token_count, 2 * inner), BF16)],
    )
    chip = add(keep, exchange(send, "tp", 1))
    mixed = call(mixed_kernel, shape(half, width), [chip, exchange(chip, "tp", 2), row, gain], held=(2, 3))
    others = exchange(mixed, "tp", 1)
    sizes = [shape(rows, width)] * len(near) + [shape(rows // 2, width)] * len(far)
    sent = call(
        part(dispatch_kernel, CAP, experts), sizes, [mixed, others, codes],
        scratch=[pltpu.VMEM((token_count, width), BF16)],
    )
    got = {k: exchange(sent[k], "sp", k) for k in everyone[1:]}
    close, remote = far[: len(far) // 2], far[len(far) // 2 :]
    block = rows // 2
    one = call(part(stack_kernel, experts, 0), shape(block * len(remote), width), [got[k] for k in remote])
    two = exchange(one, "tp", 2)
    whole, three = call(
        part(stack_kernel, experts, len(near)),
        [shape(rows * len(near), width), shape(block * len(close), width)],
        [sent[0]] + [got[k] for k in near[1:]] + [got[k] for k in close],
    )
    four = exchange(three, "tp", 2)
    mine = [whole, three, four, one, two]
    mate = [exchange(x, "tp", 1) for x in mine]
    streamed = experts - ready
    split = min(WHOLE, count - 1)
    kept = [shape(rows * split, width), shape(rows * (count - split), width)]
    keep_near, keep_far, send_near, send_far = call(
        part(expert_kernel, len(near)), [pltpu.VMEM(x.shape, BF16) for x in kept * 2],
        mine + mate + first + weights,
        flops=1 << 33, vmem=14 * MIB, held=range(10 + len(first)), hbm=range(10 + len(first), 13 + len(first)),
        scratch=[DMA((streamed, 3))] + [pltpu.VMEM((streamed,) + x.shape[1:], BF16) for x in weights],
    )
    got_far, got_near = exchange(send_far, "tp", 1), exchange(send_near, "tp", 1)
    later = range(split, count)
    pieces = [later[: len(later) // 2], later[len(later) // 2 :]]
    *others, distant = call(
        sum_far_kernel, [shape(block * len(x), width) for x in pieces + [later]], [keep_far, got_far]
    )
    others = [exchange(x, "tp", 2) for x in others]
    sent = call(part(sum_near_kernel, experts), [shape(rows, width)] * split, [keep_near, got_near])
    blocks = [sent[0]] + [exchange(sent[k], "sp", k) for k in range(1, split)]
    for n, piece in enumerate(pieces):
        sent = call(
            part(split_kernel, (piece[0] - split) * block), [shape(block, width)] * len(piece),
            [distant, others[n]],
        )
        blocks += [exchange(x, "sp", k) for x, k in zip(sent, piece)]
    send, keep = call(
        part(combine_kernel, CAP, experts, split), [shape(half, width)] * 2, blocks + [codes, gates],
        scratch=[pltpu.VMEM((token_count, width), F32)],
    )
    chip = add(keep, exchange(send, "tp", 1))
    result = call(final_kernel, shape(half, width), [chip, exchange(chip, "tp", 2), mixed, gain_two.reshape(1, -1)])
    return call(join_kernel, shape(token_count, width), [result, exchange(result, "tp", 1)])


def layer(*args):
    tokens, value_narrow, ids = args[0], args[3], args[13]
    count, tp_count = lax.axis_size("sp"), lax.axis_size("tp")
    fits = (
        tp_count == 4
        and count == 2 * (value_narrow.shape[1] // V)
        and count & (count - 1) == 0
        and QK_BROAD == V
        and 2 * QK_NARROW == V
        and tokens.shape[0] % 16 == 0
        and ids.shape[1] == TOP
        and args[15].shape[0] % 2 == 0
    )
    return (fast if fits else on_device)(*args)


def solution(mesh):
    return jax.shard_map(
        layer,
        mesh=mesh,
        in_specs=(
            P("sp", None),
            P("sp", "tp"),
            P("sp", "tp"),
            P("sp", "tp"),
            P("sp", "tp"),
            P("sp", "tp"),
            P("sp", "tp"),
            P(None, "tp"),
            P(),
            P("tp", None),
            P("tp", None),
            P(),
            P(),
            P("sp", None),
            P("sp", None),
            P("sp", None, "tp"),
            P("sp", None, "tp"),
            P("sp", "tp", None),
        ),
        out_specs=P("sp", None),
        check_vma=False,
    )
```
